256 devices in a mesh: grp: 2 (over y), sp: 16 (over z), tp: 8 (over x, core).
Axes of the slice: x: 4, y: 2, z: 16, core: 2. Of those that a mesh axis runs over, the one named last changes fastest.
The devices are a block of a 4x16x16 slice.
Arguments:
- tokens: bfloat16 [2, 16384, 2048], P('grp', ('sp', 'tp')), parts along dimension 0, may hold values from -6 to 6
- norm_gain: bfloat16 [2048], replicated, may hold values from 0.099609375 to 1.8984375
- w_query: bfloat16 [2048, 1024], P('sp'), may hold values from -0.125 to 0.125
- w_forget: bfloat16 [2048, 1024], P('sp'), may hold values from -0.125 to 0.125
- w_input: bfloat16 [2048, 1024], P('sp'), may hold values from -0.125 to 0.125
- floor_gap: float32 [1024], replicated, may hold values from 1.8310547e-05 to 0.12
- extra_decay: float32 [2, 16384, 16], P('grp', ('sp', 'tp')), parts along dimension 0, may hold values from -1.4 to 0, as said below
- init_state: float32 [2, 16, 64, 64], P('grp'), parts along dimension 0, may hold values from -0.03125 to 0.03125
- head_norm_gain: bfloat16 [1024], replicated, may hold values from 0.099609375 to 1.8984375
- w_output: bfloat16 [1024, 2048], P(None, 'sp'), may hold values from -0.1875 to 0.1875
Outputs:
- mixed: bfloat16 [2, 16384, 2048], P('grp', ('sp', 'tp')), parts along dimension 0
- final_state: float32 [2, 65536], P('grp', ('sp', 'tp')), parts along dimension 0
The draws below stay inside these ranges and needn't reach their ends.
There are 2 independent parts, one for each index of `grp`. The reference program is written for one: setup_inputs(seed, part) draws one part's arguments, and reference() takes and returns one part's arrays. A program takes and returns all parts, laid end to end along the dimension named above; an argument that names none is the same for every part. Nothing has to cross between parts.
Inputs may be any that keep to these rules, and one draw needn't show every extreme that they name: `extra_decay`: no entry is positive.
All inputs are finite; a program needn't handle non-finite values.
Results may differ from the reference program's by a relative error of at most 0.014.
Values may be sent and summed in bfloat16 or wider, within the bound.
A program may use at most 128 MiB of HBM per device.

```python
import math
import jax
import jax.numpy as jnp
from jax import lax

D = 2048
HEADS = 16
HEAD = 64
WIDTH = 1024
BLOCK = 64
SEQS = 1
SPAN = 128
POSITION_COUNT = 16384


def draw_floor_gap(key, part):
    order = jax.random.permutation(jax.random.fold_in(key, 11), HEADS)
    rapid = order < HEADS // 2
    rapid_gap = jnp.exp(jax.random.uniform(jax.random.fold_in(key, 12), (HEADS, HEAD), jnp.float32, math.log(0.04), math.log(0.12)))
    steady_gap = jnp.exp(jax.random.uniform(jax.random.fold_in(key, 13), (HEADS, HEAD), jnp.float32, math.log(0.3), 0.0)) / POSITION_COUNT
    return jnp.where(rapid[:, None], rapid_gap, steady_gap).reshape(HEADS * HEAD).astype(jnp.float32)


def draw_extra_decay(key, part):
    pieces = POSITION_COUNT // SPAN
    factor = jnp.exp(jax.random.uniform(jax.random.fold_in(key, 21), (SEQS, pieces, 1, HEADS), jnp.float32, 0.0, math.log(4.0)))
    stable_occasions = -(0.3 / POSITION_COUNT) * jnp.broadcast_to(factor, (SEQS, pieces, SPAN, HEADS)).reshape(SEQS, POSITION_COUNT, HEADS)
    spots = jax.random.randint(jax.random.fold_in(key, 22), (SEQS, 1, HEADS, 2), 0, POSITION_COUNT)
    loss_occasions = jnp.log(jax.random.uniform(jax.random.fold_in(key, 23), (SEQS, 1, HEADS, 2), jnp.float32, 0.5, 0.8))
    strike_occasions = jnp.arange(POSITION_COUNT)[None, :, None, None] == spots
    rapid_occasions = jnp.sum(jnp.where(strike_occasions, loss_occasions, 0.0), axis=3)
    return (stable_occasions + rapid_occasions).astype(jnp.float32)


def block_scale(own_key, extent, shards, smallest, largest):
    level, own = 1.0, jax.random.fold_in(own_key, 6)
    for dim, parts in shards:
        draws = jnp.exp(jax.random.uniform(jax.random.fold_in(own, dim), (parts,), jnp.float32, smallest / len(shards), largest / len(shards)))
        level = level * jnp.repeat(draws, extent[dim] // parts).reshape([-1 if axis == dim else 1 for axis in range(len(extent))])
    return level


def centred(rng, shape, scale, reach, cuts=(), held_as=jnp.bfloat16):
    level = block_scale(rng, shape, cuts, -0.22, 0.18) if cuts else 1.0
    values = jax.random.normal(rng, shape, jnp.float32) * scale * level
    return jnp.minimum(jnp.maximum(values, -reach), reach).astype(held_as)


def setup_inputs(seed: int = 0, part: int = 0) -> dict:
    splits = jax.random.split(jax.random.key(seed), 11)
    own_keys = jax.random.split(jax.random.fold_in(splits[10], part), 11)
    return {
        "tokens": centred(own_keys[0], (SEQS, POSITION_COUNT, D), 1.0, 6.0, ((1, 128),)),
        "norm_gain": jnp.clip(1.0 + 0.18 * jax.random.normal(splits[1], (D,), jnp.float32), 0.099609375, 1.8984375).astype(jnp.bfloat16),
        "w_query": centred(splits[2], (D, WIDTH), D ** -0.5, 0.125, ((0, 16),)),
        "w_forget": centred(splits[3], (D, WIDTH), D ** -0.5, 0.125, ((0, 16),)),
        "w_input": centred(splits[4], (D, WIDTH), D ** -0.5, 0.125, ((0, 16),)),
        "floor_gap": draw_floor_gap(jax.random.fold_in(splits[10], 71), part),
        "extra_decay": draw_extra_decay(jax.random.fold_in(jax.random.fold_in(splits[10], part), 71), part),
        "init_state": centred(own_keys[7], (SEQS, HEADS, HEAD, HEAD), (0.25 / POSITION_COUNT ** 0.5), 0.03125, (), jnp.float32),
        "head_norm_gain": jnp.clip(1.0 + 0.18 * jax.random.normal(splits[8], (WIDTH,), jnp.float32), 0.099609375, 1.8984375).astype(jnp.bfloat16),
        "w_output": centred(splits[9], (WIDTH, D), WIDTH ** -0.5, 0.1875, ((1, 16),)),
    }


EPSILON = 1e-05

def layer_normed(tokens, norm_gain):
    values = tokens.astype(jnp.float32)
    center = values - lax.optimization_barrier(jnp.mean(values, axis=-1, keepdims=True))
    spread = lax.optimization_barrier(jnp.mean(center * center, axis=-1, keepdims=True))
    return (center * lax.rsqrt(spread + EPSILON) * norm_gain.astype(jnp.float32)).astype(jnp.bfloat16)

def gate_terms(normed, w_query, w_forget, w_input, floor_gap, extra_decay):
    query_raw = jnp.dot(normed, w_query, preferred_element_type=jnp.float32).astype(jnp.bfloat16)
    forget_raw = jnp.dot(normed, w_forget, preferred_element_type=jnp.float32).astype(jnp.bfloat16)
    input_raw = jnp.dot(normed, w_input, preferred_element_type=jnp.float32).astype(jnp.bfloat16)
    forget_pre = forget_raw.astype(jnp.float32)
    split_shape = forget_pre.shape[:-1] + (HEADS, HEAD)
    log_keep = jnp.logaddexp(jnp.log1p(-floor_gap), jnp.log(floor_gap) + jax.nn.log_sigmoid(forget_pre))
    log_keep = log_keep.reshape(split_shape) + extra_decay[..., None]
    key_gate = (floor_gap * jax.nn.sigmoid(-forget_pre)).reshape(split_shape)
    query = jax.nn.silu(query_raw.astype(jnp.float32)).reshape(split_shape)
    values = input_raw.astype(jnp.float32).reshape(split_shape)
    return (query, key_gate, values, log_keep)

def reference(tokens, norm_gain, w_query, w_forget, w_input, floor_gap, extra_decay, init_state, head_norm_gain, w_output):
    normed = layer_normed(tokens, norm_gain)
    query, key_gate, values, log_keep = gate_terms(normed, w_query, w_forget, w_input, floor_gap, extra_decay)
    seqs, length_total = (tokens.shape[0], tokens.shape[1])
    blocks = length_total // BLOCK
    causal = lax.broadcasted_iota(jnp.int32, (BLOCK, BLOCK), 0) >= lax.broadcasted_iota(jnp.int32, (BLOCK, BLOCK), 1)
    highest = lax.Precision.HIGHEST

    def to_blocks(array):
        return jnp.moveaxis(array.reshape(seqs, blocks, BLOCK, HEADS, HEAD), 1, 0)

    def advance(state, inputs):
        q_block, k_block, v_block, l_block = inputs
        cumul = jnp.cumsum(l_block, axis=1)
        q_decayed = q_block * jnp.exp(cumul)
        key_decayed = k_block * jnp.exp(-cumul)
        scores = jnp.einsum('sthd,suhd->shtu', q_decayed, key_decayed, precision=highest)
        scores = jnp.where(causal, scores, 0.0)
        within = jnp.einsum('shtu,suhe->sthe', scores, v_block, precision=highest)
        across = jnp.einsum('sthd,shde->sthe', q_decayed, state, precision=highest)
        totals = cumul[:, -1]
        k_tail = k_block * jnp.exp(totals[:, None] - cumul)
        updated_state = jnp.exp(totals)[..., None] * state + jnp.einsum('sthd,sthe->shde', k_tail, v_block, precision=highest)
        return (updated_state, within + across)
    final_state, outputs = lax.scan(advance, init_state, (to_blocks(query), to_blocks(key_gate), to_blocks(values), to_blocks(log_keep)))
    recurrent = jnp.moveaxis(outputs, 0, 1).reshape(seqs, length_total, HEADS, HEAD)
    average_power = lax.optimization_barrier(jnp.mean(recurrent * recurrent, axis=-1, keepdims=True))
    scaled = recurrent * lax.rsqrt(average_power + EPSILON) * head_norm_gain.astype(jnp.float32).reshape(HEADS, HEAD)
    gated = scaled.reshape(seqs, length_total, HEADS * HEAD).astype(jnp.bfloat16)
    mixed = jnp.dot(gated, w_output, preferred_element_type=jnp.float32).astype(jnp.bfloat16)
    return (mixed, final_state.reshape(seqs, HEADS * HEAD * HEAD))
```

```python
import jax
import jax.numpy as jnp
from jax import lax
from jax.experimental import pallas as pl
from jax.experimental.pallas import tpu as pltpu
from jax.sharding import PartitionSpec as P

HEADS = 16
HEAD = 64
BLOCK = 64
EPSILON = 1e-05
PIECES = 4
MESH = pl.DeviceIdType.MESH
BF = jnp.bfloat16
F32 = jnp.float32
NT = (((1,), (1,)), ((), ()))
TN = (((0,), (0,)), ((), ()))


def split3(value):
    high = value.astype(BF)
    rest = value - high.astype(F32)
    middle = rest.astype(BF)
    low = (rest - middle.astype(F32)).astype(BF)
    return high, middle, low


def mm(a, b, dims=None):
    if dims is None:
        return jnp.dot(a, b, preferred_element_type=F32)
    return lax.dot_general(a, b, dims, preferred_element_type=F32)


def make_kernel(n_sp, n_tp, span, width_own, d_model):
    half = n_sp // 2
    rows_all = n_tp * span
    n_blocks = rows_all // BLOCK
    piece_rows = span // PIECES
    piece_chunks = n_sp // PIECES
    k_rows = d_model // n_sp

    def kernel(
        tok_ref, gain_ref, wq_ref, wf_ref, wi_ref, gap_ref, ext_ref, init_ref, hgain_ref, wout_ref,
        mixed_ref, final_ref,
        tokens, weights, w_out, ext_all, pad, raw, keys, cums, entering, offsets, local_out, q_glob,
        own_state, states, gated, gated_in, final_buf, final_in, prefix,
        tok_send, tok_recv, wo_send, wo_recv, z_send, z_recv, ext_send, ext_recv,
        st_send, st_recv, g_send, g_recv, f_send, f_recv,
    ):
        s = lax.axis_index("sp")
        t = lax.axis_index("tp")
        chip, core = t // 2, t % 2
        n_chips = n_tp // 2
        right = ((chip + 1) % n_chips) * 2 + core
        left = ((chip + n_chips - 1) % n_chips) * 2 + core
        across = ((chip + 2) % n_chips) * 2 + core
        partner = chip * 2 + 1 - core
        up = (s + 1) % n_sp
        down = (s + n_sp - 1) % n_sp
        lanes = pl.ds(pl.multiple_of(t * width_own, width_own), width_own)

        def at_tp(index):
            return {"tp": index}

        def at_sp(index):
            return {"sp": index}

        sent = []

        def send(src, dst, send_sem, recv_sem, where):
            copy = pltpu.make_async_remote_copy(
                src_ref=src, dst_ref=dst, send_sem=send_sem, recv_sem=recv_sem,
                device_id=where, device_id_type=MESH,
            )
            copy.start()
            sent.append(copy)

        def arrived(dst, recv_sem):
            pltpu.make_async_remote_copy(
                src_ref=dst, dst_ref=dst, send_sem=tok_send.at[0], recv_sem=recv_sem,
                device_id=at_tp(partner), device_id_type=MESH,
            ).wait_recv()

        barrier = pltpu.get_barrier_semaphore()
        for i in range(1, n_tp):
            pl.semaphore_signal(
                barrier, inc=1, device_id=at_tp((t + i) % n_tp), device_id_type=MESH
            )
        for peer in (up, down):
            pl.semaphore_signal(barrier, inc=1, device_id=at_sp(peer), device_id_type=MESH)

        own_rows = pl.ds(pl.multiple_of(s * k_rows, k_rows), k_rows)
        for m, ref in enumerate((wq_ref, wf_ref, wi_ref)):
            weights[own_rows, m * width_own : (m + 1) * width_own] = ref[:, lanes]
        w_out[t, 0] = wout_ref[pl.ds(pl.multiple_of(t * width_own, width_own), width_own), :]
        pad[...] = jnp.zeros_like(pad)
        pad[:, :HEADS] = ext_ref[...]
        ext_all[t] = pad[...].T[:HEADS]

        pl.semaphore_wait(barrier, n_tp - 1 + 2)

        def z_piece(piece, source, slot):
            if piece < 3:
                rows = pl.ds(pl.multiple_of(source * k_rows, k_rows), k_rows)
                return weights.at[rows, pl.ds(piece * width_own, width_own)]
            return w_out.at[t, slot]

        def z_own(piece):
            if piece < 3:
                return (wq_ref, wf_ref, wi_ref)[piece].at[:, lanes]
            return wout_ref.at[pl.ds(pl.multiple_of(t * width_own, width_own), width_own), :]

        def z_pieces(direction, step):
            if step < half:
                return (1, 2, 0, 3)
            return (1, 0) if direction == 0 else (2, 3)

        def z_forward(step):
            for piece in (1, 2, 0, 3):
                for direction in (0, 1):
                    if piece not in z_pieces(direction, step):
                        continue
                    if direction == 0:
                        source = (s + n_sp - (step - 1)) % n_sp
                        slot_here, slot_there = max(2 * step - 3, 0), 2 * step - 1
                    else:
                        source = (s + (step - 1)) % n_sp
                        slot_here, slot_there = 2 * step - 2, min(2 * step, n_sp - 1)
                    src = z_own(piece) if step == 1 else z_piece(piece, source, slot_here)
                    send(
                        src, z_piece(piece, source, slot_there),
                        z_send.at[direction, step - 1, piece], z_recv.at[direction, step - 1, piece],
                        at_sp(up if direction == 0 else down),
                    )

        def z_arrived(step):
            for piece in (1, 2, 0, 3):
                for direction in (0, 1):
                    if piece not in z_pieces(direction, step):
                        continue
                    if direction == 0:
                        source, slot = (s + n_sp - step) % n_sp, 2 * step - 1
                    else:
                        source, slot = (s + step) % n_sp, min(2 * step, n_sp - 1)
                    arrived(z_piece(piece, source, slot), z_recv.at[direction, step - 1, piece])

        z_forward(1)

        for i in range(1, n_tp):
            send(
                ext_all.at[t], ext_all.at[t], ext_send.at[i], ext_recv.at[t],
                at_tp((t + i) % n_tp),
            )

        for p in range(PIECES):
            here = slice(p * piece_rows, (p + 1) * piece_rows)
            values = tok_ref[here, :].astype(F32)
            center = values - jnp.mean(values, axis=-1, keepdims=True)
            spread = jnp.mean(center * center, axis=-1, keepdims=True)
            normed = center * lax.rsqrt(spread + EPSILON) * gain_ref[...].astype(F32)
            tokens[pl.ds(pl.multiple_of(t * span + p * piece_rows, piece_rows), piece_rows), :] = (
                normed.astype(BF)
            )

        def tok_piece(block, p):
            return tokens.at[
                pl.ds(pl.multiple_of(block * span + p * piece_rows, piece_rows), piece_rows), :
            ]

        def wo_piece(block, p):
            return w_out.at[block, pl.ds(p * piece_chunks, piece_chunks)]

        class Ring:
            def __init__(self, piece, send_sem, recv_sem, left_first, onward):
                self.piece, self.send_sem, self.recv_sem = piece, send_sem, recv_sem
                self.count = 0
                onward_right, onward_left = onward
                self.onward_right, self.onward_left = onward_right, onward_left
                self.from_left = [(left, p) for p in range(PIECES)] + [
                    (across, p) for p in onward_right
                ]
                self.from_right = [(right, p) for p in left_first] + [
                    (across, p) for p in onward_left
                ]

            def push(self, block, p, where):
                send(
                    self.piece(block, p), self.piece(block, p),
                    self.send_sem.at[self.count], self.recv_sem.at[block, p], at_tp(where),
                )
                self.count += 1

            def take(self, j):
                for number, (block, p) in enumerate((self.from_left[j], self.from_right[j])):
                    arrived(self.piece(block, p), self.recv_sem.at[block, p])
                    if number == 0 and j < PIECES and p in self.onward_right:
                        self.push(block, p, right)
                    if number == 1 and j < PIECES and p in self.onward_left:
                        self.push(block, p, left)
                    self.push(block, p, partner)

            def partners(self):
                for where in (0, 1, n_chips - 1, 2):
                    block = ((chip + where) % n_chips) * 2 + 1 - core
                    for p in range(PIECES):
                        arrived(self.piece(block, p), self.recv_sem.at[block, p])

        tok_ring = Ring(tok_piece, tok_send, tok_recv, (2, 3, 0, 1), ((0, 1), (2, 3)))
        for p, q in zip((0, 1, 2, 3), (2, 3, 0, 1)):
            tok_ring.push(t, p, right)
            tok_ring.push(t, q, left)
        for p in range(PIECES):
            tok_ring.push(t, p, partner)
        wo_ring = Ring(wo_piece, wo_send, wo_recv, (0, 1, 2, 3), ((0, 1), (2, 3)))

        def wo_push(p):
            wo_ring.push(t, p, right)
            wo_ring.push(t, p, left)
            wo_ring.push(t, p, partner)

        ready = [((p + 1) * piece_chunks) // 2 for p in range(PIECES)]
        taken = 0
        for step in range(1, half + 1):
            z_arrived(step)
            if step < half:
                z_forward(step + 1)
            while taken < 6 and (taken < step or step == half):
                tok_ring.take(taken)
                taken += 1
            for p in range(PIECES):
                if ready[p] == step or (ready[p] == 0 and step == 1):
                    wo_push(p)
        tok_ring.partners()
        for i in range(1, n_tp):
            arrived(ext_all.at[(t + i) % n_tp], ext_recv.at[(t + i) % n_tp])

        rows_step = 256
        for r in range(0, rows_all, rows_step):
            raw[r : r + rows_step, :] = mm(tokens[r : r + rows_step, :], weights[...]).astype(BF)

        gap = gap_ref[:, lanes]
        row_i = lax.broadcasted_iota(jnp.int32, (2 * BLOCK, 2 * BLOCK), 0)
        col_i = lax.broadcasted_iota(jnp.int32, (2 * BLOCK, 2 * BLOCK), 1)
        causal = jnp.logical_and(row_i >= col_i, row_i // BLOCK == col_i // BLOCK)
        tri = jnp.where(causal, 1.0, 0.0).astype(BF)
        tri3 = jnp.concatenate([tri, tri, tri], axis=1)
        head_row = lax.broadcasted_iota(jnp.int32, (HEADS, width_own), 0)
        head_col = lax.broadcasted_iota(jnp.int32, (HEADS, width_own), 1)
        pick = jnp.where(
            head_row == t * (width_own // HEAD) + head_col // HEAD, 1.0, 0.0
        ).astype(BF)
        pick3 = jnp.concatenate([pick, pick, pick], axis=0)
        for i in range(n_tp):
            here = slice(i * span, (i + 1) * span)
            forget = raw[here, width_own : 2 * width_own].astype(F32)
            key = gap / (1.0 + jnp.exp(forget))
            extra = mm(jnp.concatenate(split3(ext_all[i]), axis=0), pick3, TN)
            log_keep = jnp.log1p(-key) + extra
            cums[here, :] = mm(tri3, jnp.concatenate(split3(log_keep), axis=0))
            keys[here, :] = key

        lane = lax.broadcasted_iota(jnp.int32, (HEAD, width_own), 1)
        first = lane < HEAD
        state = jnp.zeros((HEAD, width_own), F32)
        offset = jnp.zeros((1, width_own), F32)
        for b in range(n_blocks):
            here = slice(b * BLOCK, (b + 1) * BLOCK)
            total = cums[(b + 1) * BLOCK - 1 : (b + 1) * BLOCK, :]
            tail = (keys[here, :] * jnp.exp(total - cums[here, :])).astype(BF)
            added = mm(raw[here, 2 * width_own :], tail, TN)
            entering[b] = state.astype(BF)
            offsets[b] = offset
            state = state * jnp.exp(total) + jnp.where(first, added[:HEAD], added[HEAD:])
            offset = offset + total
        own_state[:HEAD] = state.astype(BF)
        o_high, o_middle, o_low = split3(offset)
        log_row = lax.broadcasted_iota(jnp.int32, (16, width_own), 0)
        own_state[HEAD:] = jnp.where(
            log_row == 0, o_high.astype(F32),
            jnp.where(log_row == 1, o_middle.astype(F32),
                      jnp.where(log_row == 2, o_low.astype(F32), 0.0)),
        ).astype(BF)
        states[s] = own_state[...]

        order = [half]
        for k in range(half - 1, 0, -1):
            order += [k, n_sp - k]
        for k in order:
            send(
                own_state, states.at[s], st_send.at[k], st_recv.at[s], at_sp((s + k) % n_sp),
            )

        for j in range(3):
            wo_ring.take(j)

        lane2 = lax.broadcasted_iota(jnp.int32, (span, width_own), 1)
        first2 = lane2 < HEAD

        def spread_heads(value, mask):
            zero = jnp.zeros_like(value)
            return jnp.concatenate(
                [jnp.where(mask, value, zero), jnp.where(mask, zero, value)], axis=0
            )

        for i in range(n_tp):
            here = slice(i * span, (i + 1) * span)
            query = raw[here, :width_own].astype(F32)
            query = query / (1.0 + jnp.exp(-query))
            cumul = cums[here, :]
            q_decayed = query * jnp.exp(cumul)
            k_decayed = (keys[here, :] * jnp.exp(-cumul)).astype(BF)
            scores = mm(spread_heads(q_decayed, first2).astype(BF), k_decayed, NT)
            scores = jnp.where(jnp.concatenate([causal, causal], axis=0), scores, 0.0)
            within = mm(scores.astype(BF), raw[here, 2 * width_own :])
            within = jnp.where(first2, within[:span], within[span:])
            for j in range(span // BLOCK):
                b = i * (span // BLOCK) + j
                part = slice(j * BLOCK, (j + 1) * BLOCK)
                q_part = q_decayed[part]
                seen = mm(
                    q_part.astype(BF), spread_heads(entering[b].astype(F32), first).astype(BF), NT
                )
                rows = slice(b * BLOCK, (b + 1) * BLOCK)
                local_out[rows, :] = within[part] + seen
                q_glob[rows, :] = (q_part * jnp.exp(offsets[b])).astype(BF)

        wo_ring.take(3)

        pad[...] = jnp.zeros_like(pad)
        pad[:, :HEAD] = init_ref[
            pl.ds(pl.multiple_of(t * width_own, width_own), width_own), :
        ]
        carried = pad[...].T[:HEAD]
        for k in range(1, n_sp):
            other = (s + k) % n_sp
            arrived(states.at[other], st_recv.at[other])

        def advance(j, value):
            logs = states[j, HEAD:].astype(F32)
            total = logs[0:1] + logs[1:2] + logs[2:3]
            return value * jnp.exp(total) + states[j, :HEAD].astype(F32)

        carried = lax.fori_loop(0, s, advance, carried)
        prefix[...] = spread_heads(carried, first).astype(BF)

        ones_row = lax.broadcasted_iota(jnp.int32, (width_own, width_own), 0)
        ones_col = lax.broadcasted_iota(jnp.int32, (width_own, width_own), 1)
        same = jnp.where(ones_row // HEAD == ones_col // HEAD, 1.0 / HEAD, 0.0).astype(BF)
        same2 = jnp.concatenate([same, same], axis=0)
        head_gain = hgain_ref[:, lanes].astype(F32)
        for i in range(1, n_tp + 1):
            block = (t + i) % n_tp
            rows = pl.ds(pl.multiple_of(block * span, span), span)
            recurrent = local_out[rows, :] + mm(q_glob[rows, :], prefix[...], NT)
            square = recurrent * recurrent
            high = square.astype(BF)
            low = (square - high.astype(F32)).astype(BF)
            power = mm(jnp.concatenate([high, low], axis=1), same2)
            done = (recurrent * lax.rsqrt(power + EPSILON) * head_gain).astype(BF)
            if i < n_tp:
                gated[rows, :] = done
                send(
                    gated.at[rows, :], gated_in.at[:, lanes], g_send.at[i], g_recv.at[t],
                    at_tp(block),
                )
            else:
                gated_in[:, lanes] = done

        if HEADS == n_sp:
            keeper = s // (HEADS // n_tp)
            sub = (s % (HEADS // n_tp)) * HEAD
            part_rows = HEAD // n_tp

            @pl.when(t == keeper)
            def _():
                last = lax.fori_loop(s, n_sp, advance, carried)
                turned = jnp.concatenate([last, last], axis=0).T
                final_buf[...] = turned
                final_in[...] = final_buf[
                    pl.ds(pl.multiple_of(sub + t * part_rows, part_rows), part_rows), :
                ]
                mine = []
                for i in range(1, n_tp):
                    other = (t + i) % n_tp
                    copy = pltpu.make_async_remote_copy(
                        src_ref=final_buf.at[
                            pl.ds(pl.multiple_of(sub + other * part_rows, part_rows), part_rows), :
                        ],
                        dst_ref=final_in, send_sem=f_send.at[i], recv_sem=f_recv,
                        device_id=at_tp(other), device_id_type=MESH,
                    )
                    copy.start()
                    mine.append(copy)
                for copy in mine:
                    copy.wait_send()

            @pl.when(t != keeper)
            def _():
                arrived(final_in, f_recv)

            for r in range(part_rows):
                final_ref[:, r * HEAD : (r + 1) * HEAD] = final_in[r : r + 1, :HEAD]

        wo_ring.take(4)
        wo_ring.take(5)
        wo_ring.partners()
        for i in range(1, n_tp):
            other = (t + i) % n_tp
            arrived(
                gated_in.at[:, pl.ds(pl.multiple_of(other * width_own, width_own), width_own)],
                g_recv.at[other],
            )

        def source_of(slot):
            step = (slot + 1) // 2
            return (s + n_sp - step) % n_sp if slot % 2 else (s + step) % n_sp

        for pair in range(n_sp // 2):
            right_side = jnp.concatenate(
                [w_out[:, slot].reshape(n_tp * width_own, -1) for slot in (2 * pair, 2 * pair + 1)],
                axis=1,
            )
            product = mm(gated_in[...], right_side).astype(BF)
            cols = product.shape[1] // 2
            for k in range(2):
                source = source_of(2 * pair + k)
                mixed_ref[:, pl.ds(pl.multiple_of(source * cols, cols), cols)] = (
                    product[:, k * cols : (k + 1) * cols]
                )
        for copy in sent:
            copy.wait_send()

    return kernel


def solution(mesh):
    n_sp, n_tp = mesh.shape["sp"], mesh.shape["tp"]

    def body(
        tokens, norm_gain, w_query, w_forget, w_input, floor_gap, extra_decay, init_state,
        head_norm_gain, w_output,
    ):
        span, d_model = tokens.shape[1], tokens.shape[2]
        width = w_query.shape[1]
        own = width // n_tp
        rows = n_tp * span
        blocks = rows // BLOCK
        flat = HEADS * HEAD * HEAD // (n_sp * n_tp)
        vmem = pl.BlockSpec(memory_space=pltpu.VMEM)
        dma = pltpu.SemaphoreType.DMA
        mixed, final_state = pl.pallas_call(
            make_kernel(n_sp, n_tp, span, own, d_model),
            out_shape=(
                jax.ShapeDtypeStruct((span, d_model), BF),
                jax.ShapeDtypeStruct((1, flat), F32),
            ),
            in_specs=[vmem] * 10,
            out_specs=(vmem, vmem),
            scratch_shapes=[
                pltpu.VMEM((rows, d_model), BF),
                pltpu.VMEM((d_model, 3 * own), BF),
                pltpu.VMEM((n_tp, n_sp, own, d_model // n_sp), BF),
                pltpu.VMEM((n_tp, HEADS, span), F32),
                pltpu.VMEM((span, own), F32),
                pltpu.VMEM((rows, 3 * own), BF),
                pltpu.VMEM((rows, own), F32),
                pltpu.VMEM((rows, own), F32),
                pltpu.VMEM((blocks, HEAD, own), BF),
                pltpu.VMEM((blocks, 1, own), F32),
                pltpu.VMEM((rows, own), F32),
                pltpu.VMEM((rows, own), BF),
                pltpu.VMEM((HEAD + 16, own), BF),
                pltpu.VMEM((n_sp, HEAD + 16, own), BF),
                pltpu.VMEM((rows, own), BF),
                pltpu.VMEM((span, width), BF),
                pltpu.VMEM((own, 2 * HEAD), F32),
                pltpu.VMEM((HEAD // n_tp, 2 * HEAD), F32),
                pltpu.VMEM((own, own), BF),
                dma((28,)), dma((n_tp, PIECES)), dma((28,)), dma((n_tp, PIECES)),
                dma((2, n_sp // 2, 4)), dma((2, n_sp // 2, 4)),
                dma((n_tp,)), dma((n_tp,)),
                dma((n_sp,)), dma((n_sp,)),
                dma((n_tp,)), dma((n_tp,)),
                dma((n_tp,)), dma,
            ],
            compiler_params=pltpu.CompilerParams(
                collective_id=0, has_side_effects=True, vmem_limit_bytes=56 * 1024 * 1024
            ),
            name="mixer",
        )(
            tokens.reshape(span, d_model),
            norm_gain.reshape(1, d_model),
            w_query, w_forget, w_input,
            floor_gap.reshape(1, width),
            extra_decay.reshape(span, HEADS),
            init_state.reshape(HEADS * HEAD, HEAD),
            head_norm_gain.reshape(1, width),
            w_output,
        )
        return mixed.reshape(1, span, d_model), final_state

    in_specs = (
        P("grp", ("sp", "tp"), None),
        P(),
        P("sp", None),
        P("sp", None),
        P("sp", None),
        P(),
        P("grp", ("sp", "tp"), None),
        P("grp", None, None, None),
        P(),
        P(None, "sp"),
    )
    out_specs = (P("grp", ("sp", "tp"), None), P("grp", ("sp", "tp")))
    return jax.shard_map(body, mesh=mesh, in_specs=in_specs, out_specs=out_specs, check_vma=False)
```

```python
import jax
import jax.numpy as jnp
from jax import lax
from jax.experimental import pallas as pl
from jax.experimental.pallas import tpu as pltpu
from jax.sharding import PartitionSpec as P

HEADS = 16
HEAD = 64
BLOCK = 64
EPSILON = 1e-05
PIECES = 4
LAG = 2
LOG_ROWS = 8
MESH = pl.DeviceIdType.MESH
BF = jnp.bfloat16
F32 = jnp.float32
NT = (((1,), (1,)), ((), ()))
TN = (((0,), (0,)), ((), ()))


def split3(value):
    high = value.astype(BF)
    rest = value - high.astype(F32)
    middle = rest.astype(BF)
    low = (rest - middle.astype(F32)).astype(BF)
    return high, middle, low


def mm(a, b, dims=None):
    if dims is None:
        return jnp.dot(a, b, preferred_element_type=F32)
    return lax.dot_general(a, b, dims, preferred_element_type=F32)


def make_kernel(n_sp, n_tp, span, width_own, d_model):
    half = n_sp // 2
    rows_all = n_tp * span
    n_blocks = rows_all // BLOCK
    piece_rows = span // PIECES
    piece_chunks = n_sp // PIECES
    k_rows = d_model // n_sp

    def kernel(
        tok_ref, gain_ref, wq_ref, wf_ref, wi_ref, gap_ref, ext_ref, init_ref, hgain_ref, wout_ref,
        mixed_ref, final_ref,
        tok_in, init_in, tokens, weights, others, w_out, ext_all, pad, raw, keys, cums, entering,
        offsets, local_out, q_glob, own_state, states, gated, gated_in, final_buf, final_in, prefix,
        load_sem, tok_send, tok_recv, wo_send, wo_recv, z_send, z_recv, zo_send, zo_recv,
        d_send, d_recv, do_send, do_recv, ext_send, ext_recv,
        st_send, st_recv, g_send, g_recv, f_send, f_recv,
    ):
        s = lax.axis_index("sp")
        t = lax.axis_index("tp")
        chip, core = t // 2, t % 2
        n_chips = n_tp // 2
        right = ((chip + 1) % n_chips) * 2 + core
        left = ((chip + n_chips - 1) % n_chips) * 2 + core
        across = ((chip + 2) % n_chips) * 2 + core
        partner = chip * 2 + 1 - core
        onto = (s + n_sp + 1 - 2 * core) % n_sp
        behind = (s + n_sp - 1 + 2 * core) % n_sp
        lanes = pl.ds(pl.multiple_of(t * width_own, width_own), width_own)
        lanes_partner = pl.ds(pl.multiple_of(partner * width_own, width_own), width_own)

        def at_tp(index):
            return {"tp": index}

        def at_sp(index):
            return {"sp": index}

        sent = []

        def send(src, dst, send_sem, recv_sem, where):
            copy = pltpu.make_async_remote_copy(
                src_ref=src, dst_ref=dst, send_sem=send_sem, recv_sem=recv_sem,
                device_id=where, device_id_type=MESH,
            )
            copy.start()
            sent.append(copy)

        def arrived(dst, recv_sem):
            pltpu.make_async_remote_copy(
                src_ref=dst, dst_ref=dst, send_sem=tok_send.at[0], recv_sem=recv_sem,
                device_id=at_tp(partner), device_id_type=MESH,
            ).wait_recv()

        barrier = pltpu.get_barrier_semaphore()
        for i in range(1, n_tp):
            pl.semaphore_signal(
                barrier, inc=1, device_id=at_tp((t + i) % n_tp), device_id_type=MESH
            )
        pl.semaphore_signal(barrier, inc=1, device_id=at_sp(behind), device_id_type=MESH)

        def source_at(step):
            return (s + n_sp - step + 2 * core * step) % n_sp

        def source_beside(step):
            return (s + n_sp + step - 2 * core * step) % n_sp

        def slot_at(step):
            if step == 0:
                return 0
            return n_sp - 1 if step == half else 2 * step - 1 + core

        def w_piece(ref, source, m):
            rows = pl.ds(pl.multiple_of(source * k_rows, k_rows), k_rows)
            return ref.at[rows, pl.ds(m * width_own, width_own)]

        def own_channels(index):
            return pl.ds(pl.multiple_of(index * width_own, width_own), width_own)

        loads = []

        def load(src, dst):
            copy = pltpu.make_async_copy(src, dst, load_sem.at[len(loads)])
            copy.start()
            loads.append(copy)

        load(tok_ref, tok_in)
        for m, ref in enumerate((wq_ref, wf_ref, wi_ref)):
            load(ref.at[:, lanes_partner], w_piece(others, s, m))
            load(ref.at[:, lanes], w_piece(weights, s, m))
        load(ext_ref, ext_all.at[t])
        load(wout_ref.at[own_channels(t), :], w_out.at[t, 0])
        load(wout_ref.at[own_channels(partner), :], w_out.at[partner, 0])
        load(init_ref.at[own_channels(t), :], init_in)

        loads[0].wait()
        gain = gain_ref[...].astype(F32).reshape(1, d_model)
        for p in range(PIECES):
            here = slice(p * piece_rows, (p + 1) * piece_rows)
            values = tok_in[here, :].astype(F32)
            center = values - jnp.mean(values, axis=-1, keepdims=True)
            spread = jnp.mean(center * center, axis=-1, keepdims=True)
            normed = center * lax.rsqrt(spread + EPSILON) * gain
            tokens[pl.ds(pl.multiple_of(t * span + p * piece_rows, piece_rows), piece_rows), :] = (
                normed.astype(BF)
            )
        for copy in loads[1:]:
            copy.wait()

        pl.semaphore_wait(barrier, n_tp - 1 + 1)

        def z_items(step):
            return [(m, part) for m in (1, 2, 0) for part in ((1, 0) if step < half else (0,))]

        def z_push(step, m, part):
            ref = others if part else weights
            piece = w_piece(ref, source_at(step - 1), m)
            send(
                piece, piece, z_send.at[step - 1, m, part], z_recv.at[step - 1, m, part],
                at_sp(onto),
            )

        def z_step(step):
            for m, part in z_items(step):
                piece = w_piece(others if part else weights, source_at(step), m)
                arrived(piece, z_recv.at[step - 1, m, part])
                if step < half and (m, part) in z_items(step + 1):
                    z_push(step + 1, m, part)
                if part:
                    send(
                        piece, w_piece(weights, source_at(step), m), d_send.at[step - 1, m],
                        d_recv.at[step - 1, m], at_tp(partner),
                    )

        def zo_parts(step):
            return (1, 0) if step < half else (0,)

        def zo_push(step, part):
            block = partner if part else t
            send(
                w_out.at[block, slot_at(step - 1)], w_out.at[block, slot_at(step)],
                zo_send.at[step - 1, part], zo_recv.at[step - 1, part], at_sp(onto),
            )

        def zo_step(step):
            if step == 0:
                for part in (1, 0):
                    zo_push(1, part)
                return
            for part in zo_parts(step):
                piece = w_out.at[partner if part else t, slot_at(step)]
                arrived(piece, zo_recv.at[step - 1, part])
                if step < half and part in zo_parts(step + 1):
                    zo_push(step + 1, part)
                send(
                    piece, piece, do_send.at[step - 1, part], do_recv.at[step - 1, part],
                    at_tp(partner),
                )

        def zo_beside(step, part):
            slot = n_sp - 1 if step == half else 2 * step - core
            arrived(w_out.at[t if part else partner, slot], do_recv.at[step - 1, part])

        for m, part in z_items(1):
            z_push(1, m, part)

        def tok_piece(block, p):
            return tokens.at[
                pl.ds(pl.multiple_of(block * span + p * piece_rows, piece_rows), piece_rows), :
            ]

        def wo_piece(block, p):
            return w_out.at[block, pl.ds(p * piece_chunks, piece_chunks)]

        class Ring:
            def __init__(self, piece, send_sem, recv_sem, left_first, onward):
                self.piece, self.send_sem, self.recv_sem = piece, send_sem, recv_sem
                self.count = 0
                onward_right, onward_left = onward
                self.onward_right, self.onward_left = onward_right, onward_left
                self.from_left = [(left, p) for p in range(PIECES)] + [
                    (across, p) for p in onward_right
                ]
                self.from_right = [(right, p) for p in left_first] + [
                    (across, p) for p in onward_left
                ]

            def push(self, block, p, where):
                send(
                    self.piece(block, p), self.piece(block, p),
                    self.send_sem.at[self.count], self.recv_sem.at[block, p], at_tp(where),
                )
                self.count += 1

            def take(self, j):
                for number, (block, p) in enumerate((self.from_left[j], self.from_right[j])):
                    arrived(self.piece(block, p), self.recv_sem.at[block, p])
                    if number == 0 and j < PIECES and p in self.onward_right:
                        self.push(block, p, right)
                    if number == 1 and j < PIECES and p in self.onward_left:
                        self.push(block, p, left)
                    self.push(block, p, partner)

            def partners(self, chips):
                for where in chips:
                    block = ((chip + where) % n_chips) * 2 + 1 - core
                    for p in range(PIECES):
                        arrived(self.piece(block, p), self.recv_sem.at[block, p])

        for i in range(1, n_tp):
            send(
                ext_all.at[t], ext_all.at[t], ext_send.at[i], ext_recv.at[t],
                at_tp((t + i) % n_tp),
            )
        tok_ring = Ring(tok_piece, tok_send, tok_recv, (2, 3, 0, 1), ((0, 1), (2, 3)))
        for p, q in zip((0, 1, 2, 3), (2, 3, 0, 1)):
            tok_ring.push(t, p, right)
            tok_ring.push(t, q, left)
        for p in range(PIECES):
            tok_ring.push(t, p, partner)
        wo_ring = Ring(wo_piece, wo_send, wo_recv, (0, 1, 2, 3), ((0, 1), (2, 3)))

        ready = [((p + 1) * piece_chunks) // 2 for p in range(PIECES)]
        pushed = [0, 0]

        def wo_advance(step):
            while pushed[0] < PIECES and ready[pushed[0]] < step:
                while pushed[1] < ready[pushed[0]]:
                    pushed[1] += 1
                    for part in reversed(zo_parts(pushed[1])):
                        zo_beside(pushed[1], part)
                wo_ring.push(t, pushed[0], right)
                wo_ring.push(t, pushed[0], left)
                pushed[0] += 1
            if step <= half:
                zo_step(step)

        taken = 0
        for step in range(1, half + 1):
            z_step(step)
            while taken < 6 and (taken < step or step == half):
                tok_ring.take(taken)
                taken += 1
            if step >= LAG:
                wo_advance(step - LAG)
        for step in range(1, half):
            for m in range(3):
                arrived(w_piece(weights, source_beside(step), m), d_recv.at[step - 1, m])
        tok_ring.partners((0, 1, n_chips - 1, 2))
        for i in range(1, n_tp):
            arrived(ext_all.at[(t + i) % n_tp], ext_recv.at[(t + i) % n_tp])

        rows_step = 256
        for r in range(0, rows_all, rows_step):
            raw[r : r + rows_step, :] = mm(tokens[r : r + rows_step, :], weights[...]).astype(BF)

        wo_advance(half - LAG + 1)
        gap = gap_ref[:, lanes]
        row_i = lax.broadcasted_iota(jnp.int32, (2 * BLOCK, 2 * BLOCK), 0)
        col_i = lax.broadcasted_iota(jnp.int32, (2 * BLOCK, 2 * BLOCK), 1)
        causal = jnp.logical_and(row_i >= col_i, row_i // BLOCK == col_i // BLOCK)
        tri = jnp.where(causal, 1.0, 0.0).astype(BF)
        tri3 = jnp.concatenate([tri, tri, tri], axis=1)
        head_row = lax.broadcasted_iota(jnp.int32, (HEADS, width_own), 0)
        head_col = lax.broadcasted_iota(jnp.int32, (HEADS, width_own), 1)
        pick = jnp.where(
            head_row == t * (width_own // HEAD) + head_col // HEAD, 1.0, 0.0
        ).astype(BF)
        pick3 = jnp.concatenate([pick, pick, pick], axis=0)
        for i in range(n_tp):
            here = slice(i * span, (i + 1) * span)
            forget = raw[here, width_own : 2 * width_own].astype(F32)
            key = gap / (1.0 + jnp.exp(forget))
            extra = mm(jnp.concatenate(split3(ext_all[i]), axis=0), pick3, TN)
            log_keep = jnp.log1p(-key) + extra
            cums[here, :] = mm(tri3, jnp.concatenate(split3(log_keep), axis=0))
            keys[here, :] = key

        lane = lax.broadcasted_iota(jnp.int32, (HEAD, width_own), 1)
        first = lane < HEAD
        state = jnp.zeros((HEAD, width_own), F32)
        offset = jnp.zeros((1, width_own), F32)
        for b in range(n_blocks):
            here = slice(b * BLOCK, (b + 1) * BLOCK)
            total = cums[(b + 1) * BLOCK - 1 : (b + 1) * BLOCK, :]
            tail = (keys[here, :] * jnp.exp(total - cums[here, :])).astype(BF)
            added = mm(raw[here, 2 * width_own :], tail, TN)
            entering[b] = state.astype(BF)
            offsets[b] = offset
            state = state * jnp.exp(total) + jnp.where(first, added[:HEAD], added[HEAD:])
            offset = offset + total
        own_state[:HEAD] = state.astype(BF)
        o_high, o_middle, o_low = split3(offset)
        log_row = lax.broadcasted_iota(jnp.int32, (LOG_ROWS, width_own), 0)
        own_state[HEAD:] = jnp.where(
            log_row == 0, o_high.astype(F32),
            jnp.where(log_row == 1, o_middle.astype(F32),
                      jnp.where(log_row == 2, o_low.astype(F32), 0.0)),
        ).astype(BF)

        def state_copy(j):
            return pltpu.make_async_remote_copy(
                src_ref=own_state, dst_ref=states.at[s], send_sem=st_send.at[j],
                recv_sem=st_recv.at[s], device_id=at_sp(j), device_id_type=MESH,
            )

        def state_push(k, carry):
            state_copy(n_sp - 1 - k).start()
            return carry

        lax.fori_loop(0, n_sp - 1 - s, state_push, 0)
        for step in range(half - LAG + 2, half + 2):
            wo_advance(step)
        for j in range(2):
            wo_ring.take(j)
        lane2 = lax.broadcasted_iota(jnp.int32, (span, width_own), 1)
        first2 = lane2 < HEAD

        def spread_heads(value, mask):
            zero = jnp.zeros_like(value)
            return jnp.concatenate(
                [jnp.where(mask, value, zero), jnp.where(mask, zero, value)], axis=0
            )

        for i in range(n_tp):
            here = slice(i * span, (i + 1) * span)
            query = raw[here, :width_own].astype(F32)
            query = query / (1.0 + jnp.exp(-query))
            cumul = cums[here, :]
            q_decayed = query * jnp.exp(cumul)
            k_decayed = (keys[here, :] * jnp.exp(-cumul)).astype(BF)
            scores = mm(spread_heads(q_decayed, first2).astype(BF), k_decayed, NT)
            scores = jnp.where(jnp.concatenate([causal, causal], axis=0), scores, 0.0)
            within = mm(scores.astype(BF), raw[here, 2 * width_own :])
            within = jnp.where(first2, within[:span], within[span:])
            for j in range(span // BLOCK):
                b = i * (span // BLOCK) + j
                part = slice(j * BLOCK, (j + 1) * BLOCK)
                q_part = q_decayed[part]
                seen = mm(
                    q_part.astype(BF), spread_heads(entering[b].astype(F32), first).astype(BF), NT
                )
                rows = slice(b * BLOCK, (b + 1) * BLOCK)
                local_out[rows, :] = within[part] + seen
                q_glob[rows, :] = (q_part * jnp.exp(offsets[b])).astype(BF)

        wo_ring.take(2)
        wo_ring.take(3)

        pad[...] = jnp.zeros_like(pad)
        pad[:, :HEAD] = init_in[...]
        carried = pad[...].T[:HEAD]

        def advance(j, value):
            arrived(states.at[j], st_recv.at[j])
            logs = states[j, HEAD:].astype(F32)
            total = logs[0:1] + logs[1:2] + logs[2:3]
            return value * jnp.exp(total) + states[j, :HEAD].astype(F32)

        carried = lax.fori_loop(0, s, advance, carried)
        prefix[...] = spread_heads(carried, first).astype(BF)

        ones_row = lax.broadcasted_iota(jnp.int32, (width_own, width_own), 0)
        ones_col = lax.broadcasted_iota(jnp.int32, (width_own, width_own), 1)
        same = jnp.where(ones_row // HEAD == ones_col // HEAD, 1.0 / HEAD, 0.0).astype(BF)
        same2 = jnp.concatenate([same, same], axis=0)
        gains = hgain_ref[...].astype(F32).reshape(1, n_tp * width_own)
        head_gain = gains[:, :width_own]
        for i in range(1, n_tp):
            head_gain = jnp.where(t == i, gains[:, i * width_own : (i + 1) * width_own], head_gain)
        for i in range(1, n_tp + 1):
            block = (t + i) % n_tp
            rows = pl.ds(pl.multiple_of(block * span, span), span)
            recurrent = local_out[rows, :] + mm(q_glob[rows, :], prefix[...], NT)
            square = recurrent * recurrent
            high = square.astype(BF)
            low = (square - high.astype(F32)).astype(BF)
            power = mm(jnp.concatenate([high, low], axis=1), same2)
            done = (recurrent * lax.rsqrt(power + EPSILON) * head_gain).astype(BF)
            if i < n_tp:
                gated[rows, :] = done
                send(
                    gated.at[rows, :], gated_in.at[:, lanes], g_send.at[i], g_recv.at[t],
                    at_tp(block),
                )
            else:
                gated_in[:, lanes] = done

        part_rows = HEAD // n_tp

        def final_copies(act):
            for h in range(HEADS // n_tp):
                head = t * (HEADS // n_tp) + h
                for i in range(n_tp):
                    copy = pltpu.make_async_remote_copy(
                        src_ref=final_buf.at[pl.ds(h * HEAD + i * part_rows, part_rows), :],
                        dst_ref=final_in, send_sem=f_send.at[h, i], recv_sem=f_recv,
                        device_id={"sp": head, "tp": i}, device_id_type=MESH,
                    )
                    keeps = jnp.logical_and(head == s, t == i)
                    if act == "start":
                        pl.when(jnp.logical_not(keeps))(copy.start)

                        @pl.when(keeps)
                        def _():
                            final_in[...] = final_buf[
                                h * HEAD + i * part_rows : h * HEAD + (i + 1) * part_rows, :
                            ]
                    else:
                        pl.when(jnp.logical_not(keeps))(copy.wait_send)

        if HEADS == n_sp:

            @pl.when(s == n_sp - 1)
            def _():
                last = carried * jnp.exp(offset) + state
                final_buf[...] = jnp.concatenate([last, last], axis=0).T
                final_copies("start")

        wo_ring.take(4)
        wo_ring.take(5)
        wo_ring.partners((1, n_chips - 1, 2))
        for step in range(1, half + 1):
            for part in zo_parts(step):
                if step > pushed[1]:
                    zo_beside(step, part)
        for i in range(1, n_tp):
            other = (t + i) % n_tp
            arrived(
                gated_in.at[:, pl.ds(pl.multiple_of(other * width_own, width_own), width_own)],
                g_recv.at[other],
            )

        def source_of(slot):
            step = (slot + 1) // 2
            return (s + n_sp - step) % n_sp if slot % 2 else (s + step) % n_sp

        for pair in range(n_sp // 2):
            right_side = jnp.concatenate(
                [w_out[:, slot].reshape(n_tp * width_own, -1) for slot in (2 * pair, 2 * pair + 1)],
                axis=1,
            )
            product = mm(gated_in[...], right_side).astype(BF)
            cols = product.shape[1] // 2
            for k in range(2):
                source = source_of(2 * pair + k)
                mixed_ref[:, pl.ds(pl.multiple_of(source * cols, cols), cols)] = (
                    product[:, k * cols : (k + 1) * cols]
                )
        if HEADS == n_sp:

            @pl.when(s == n_sp - 1)
            def _():
                final_copies("end")

            keeper = jnp.logical_and(s == n_sp - 1, t == s // (HEADS // n_tp))

            @pl.when(jnp.logical_not(keeper))
            def _():
                arrived(final_in, f_recv)

            for r in range(part_rows):
                final_ref[:, r * HEAD : (r + 1) * HEAD] = final_in[r : r + 1, :HEAD]

        def state_end(k, carry):
            state_copy(n_sp - 1 - k).wait_send()
            return carry

        lax.fori_loop(0, n_sp - 1 - s, state_end, 0)
        for copy in sent:
            copy.wait_send()

    return kernel


def solution(mesh):
    n_sp, n_tp = mesh.shape["sp"], mesh.shape["tp"]

    def body(
        tokens, norm_gain, w_query, w_forget, w_input, floor_gap, extra_decay, init_state,
        head_norm_gain, w_output,
    ):
        span, d_model = tokens.shape[1], tokens.shape[2]
        width = w_query.shape[1]
        own = width // n_tp
        rows = n_tp * span
        blocks = rows // BLOCK
        flat = HEADS * HEAD * HEAD // (n_sp * n_tp)
        vmem = pl.BlockSpec(memory_space=pltpu.VMEM)
        hbm = pl.BlockSpec(memory_space=pl.ANY)
        half = n_sp // 2
        dma = pltpu.SemaphoreType.DMA
        mixed, final_state = pl.pallas_call(
            make_kernel(n_sp, n_tp, span, own, d_model),
            out_shape=(
                jax.ShapeDtypeStruct((span, d_model), BF),
                jax.ShapeDtypeStruct((1, flat), F32),
            ),
            in_specs=[hbm, vmem, hbm, hbm, hbm, vmem, hbm, hbm, vmem, hbm],
            out_specs=(vmem, vmem),
            scratch_shapes=[
                pltpu.VMEM((span, d_model), BF),
                pltpu.VMEM((own, HEAD), F32),
                pltpu.VMEM((rows, d_model), BF),
                pltpu.VMEM((d_model, 3 * own), BF),
                pltpu.VMEM((d_model, 3 * own), BF),
                pltpu.VMEM((n_tp, n_sp, own, d_model // n_sp), BF),
                pltpu.VMEM((n_tp, HEADS, span), F32),
                pltpu.VMEM((span, own), F32),
                pltpu.VMEM((rows, 3 * own), BF),
                pltpu.VMEM((rows, own), F32),
                pltpu.VMEM((rows, own), F32),
                pltpu.VMEM((blocks, HEAD, own), BF),
                pltpu.VMEM((blocks, 1, own), F32),
                pltpu.VMEM((rows, own), F32),
                pltpu.VMEM((rows, own), BF),
                pltpu.VMEM((HEAD + LOG_ROWS, own), BF),
                pltpu.VMEM((n_sp, HEAD + LOG_ROWS, own), BF),
                pltpu.VMEM((rows, own), BF),
                pltpu.VMEM((span, width), BF),
                pltpu.VMEM((own, 2 * HEAD), F32),
                pltpu.VMEM((HEAD // n_tp, 2 * HEAD), F32),
                pltpu.VMEM((own, own), BF),
                dma((11,)),
                dma((28,)), dma((n_tp, PIECES)), dma((28,)), dma((n_tp, PIECES)),
                dma((half, 3, 2)), dma((half, 3, 2)), dma((half, 2)), dma((half, 2)),
                dma((half, 3)), dma((half, 3)), dma((half, 2)), dma((half, 2)),
                dma((n_tp,)), dma((n_tp,)),
                dma((n_sp,)), dma((n_sp,)),
                dma((n_tp,)), dma((n_tp,)),
                dma((HEADS // n_tp, n_tp)), dma,
            ],
            compiler_params=pltpu.CompilerParams(
                collective_id=0, has_side_effects=True, vmem_limit_bytes=56 * 1024 * 1024
            ),
            name="mixer",
        )(
            tokens.reshape(span, d_model),
            norm_gain,
            w_query, w_forget, w_input,
            floor_gap.reshape(1, width),
            jnp.swapaxes(extra_decay, 1, 2).reshape(HEADS, span),
            init_state.reshape(HEADS * HEAD, HEAD),
            head_norm_gain,
            w_output,
        )
        return mixed.reshape(1, span, d_model), final_state

    in_specs = (
        P("grp", ("sp", "tp"), None),
        P(),
        P("sp", None),
        P("sp", None),
        P("sp", None),
        P(),
        P("grp", ("sp", "tp"), None),
        P("grp", None, None, None),
        P(),
        P(None, "sp"),
    )
    out_specs = (P("grp", ("sp", "tp"), None), P("grp", ("sp", "tp")))
    return jax.shard_map(body, mesh=mesh, in_specs=in_specs, out_specs=out_specs, check_vma=False)
```

```python
import jax
import jax.numpy as jnp
from jax import lax
from jax.experimental import pallas as pl
from jax.experimental.pallas import tpu as pltpu
from jax.sharding import PartitionSpec as P

HEADS = 16
HEAD = 64
BLOCK = 64
EPSILON = 1e-05
PIECES = 4
LOG_ROWS = 8
MESH = pl.DeviceIdType.MESH
BF = jnp.bfloat16
F32 = jnp.float32
NT = (((1,), (1,)), ((), ()))
TN = (((0,), (0,)), ((), ()))


def split3(value):
    high = value.astype(BF)
    rest = value - high.astype(F32)
    middle = rest.astype(BF)
    low = (rest - middle.astype(F32)).astype(BF)
    return high, middle, low


def mm(a, b, dims=None):
    if dims is None:
        return jnp.dot(a, b, preferred_element_type=F32)
    return lax.dot_general(a, b, dims, preferred_element_type=F32)


def make_kernel(n_sp, n_tp, span, width_own, d_model):
    half = n_sp // 2
    rows_all = n_tp * span
    n_blocks = rows_all // BLOCK
    piece_rows = span // PIECES
    piece_chunks = n_sp // PIECES
    k_rows = d_model // n_sp

    def kernel(
        tok_ref, gain_ref, wq_ref, wf_ref, wi_ref, gap_ref, ext_ref, init_ref, hgain_ref, wout_ref,
        mixed_ref, final_ref,
        tok_in, gain_in, gain_rows, gap_in, hgain_in, init_in, tokens, weights, others, w_out, ext_all, pad, pick, early, raw, keys, cums, entering,
        offsets, local_out, q_glob, own_state, pair_in, pair_state, states, gated, gated_in, final_buf, final_in, prefix,
        load_sem, tok_send, tok_recv, wo_send, wo_recv, z_send, z_recv, zo_send, zo_recv,
        d_send, d_recv, do_send, do_recv, ext_send, ext_recv,
        pair_send, pair_recv, st_send, st_recv, g_send, g_recv, f_send, f_recv,
    ):
        s = lax.axis_index("sp")
        t = lax.axis_index("tp")
        chip, core = t // 2, t % 2
        n_chips = n_tp // 2
        right = ((chip + 1) % n_chips) * 2 + core
        left = ((chip + n_chips - 1) % n_chips) * 2 + core
        across = ((chip + 2) % n_chips) * 2 + core
        partner = chip * 2 + 1 - core
        onto = (s + n_sp + 1 - 2 * core) % n_sp
        behind = (s + n_sp - 1 + 2 * core) % n_sp
        lanes = pl.ds(pl.multiple_of(t * width_own, width_own), width_own)
        lanes_partner = pl.ds(pl.multiple_of(partner * width_own, width_own), width_own)

        def at_tp(index):
            return {"tp": index}

        def at_sp(index):
            return {"sp": index}

        sent = []

        def send(src, dst, send_sem, recv_sem, where):
            copy = pltpu.make_async_remote_copy(
                src_ref=src, dst_ref=dst, send_sem=send_sem, recv_sem=recv_sem,
                device_id=where, device_id_type=MESH,
            )
            copy.start()
            sent.append(copy)

        def arrived(dst, recv_sem):
            pltpu.make_async_remote_copy(
                src_ref=dst, dst_ref=dst, send_sem=tok_send.at[0], recv_sem=recv_sem,
                device_id=at_tp(partner), device_id_type=MESH,
            ).wait_recv()

        barrier = pltpu.get_barrier_semaphore()
        for i in range(1, n_tp):
            pl.semaphore_signal(
                barrier, inc=1, device_id=at_tp((t + i) % n_tp), device_id_type=MESH
            )
        pl.semaphore_signal(barrier, inc=1, device_id=at_sp(behind), device_id_type=MESH)

        def source_of(slot):
            step = (slot + 1) // 2
            return (s + n_sp - step) % n_sp if slot % 2 else (s + step) % n_sp

        def slot_at(step):
            if step == 0:
                return 0
            return n_sp - 1 if step == half else 2 * step - 1 + core

        def slot_beside(step):
            return n_sp - 1 if step == half else 2 * step - core

        def w_piece(ref, slot, m):
            start = slot * k_rows
            if not isinstance(start, int):
                start = pl.multiple_of(start, k_rows)
            return ref.at[pl.ds(start, k_rows), pl.ds(m * width_own, width_own)]

        def own_channels(index):
            return pl.ds(pl.multiple_of(index * width_own, width_own), width_own)

        loads = []

        def load(src, dst):
            copy = pltpu.make_async_copy(src, dst, load_sem.at[len(loads)])
            copy.start()
            loads.append(copy)

        load(tok_ref, tok_in)
        load(gain_ref, gain_in)
        for m, ref in enumerate((wq_ref, wf_ref, wi_ref)):
            load(ref.at[:, lanes_partner], w_piece(others, 0, m))
            load(ref.at[:, lanes], w_piece(weights, 0, m))
        load(ext_ref, ext_all.at[t])
        load(wout_ref.at[own_channels(t), :], w_out.at[t, 0])
        load(wout_ref.at[own_channels(partner), :], w_out.at[partner, 0])
        load(init_ref.at[own_channels(t), :], init_in)
        load(gap_ref, gap_in)
        load(hgain_ref, hgain_in)

        loads[0].wait()
        loads[1].wait()
        gain = gain_in[...].astype(F32).reshape(1, d_model)
        gain_rows[...] = gain
        for p in range(PIECES):
            here = slice(p * piece_rows, (p + 1) * piece_rows)
            values = tok_in[here, :].astype(F32)
            mean = jnp.mean(values, axis=-1, keepdims=True)
            center = values - mean
            scale = lax.rsqrt(jnp.mean(center * center, axis=-1, keepdims=True) + EPSILON)
            there = pl.ds(pl.multiple_of(t * span + p * piece_rows, piece_rows), piece_rows)
            for slot in range(n_sp):
                cols = pl.ds(pl.multiple_of(source_of(slot) * k_rows, k_rows), k_rows)
                normed = (tok_in[here, cols].astype(F32) - mean) * scale * gain_rows[:, cols]
                tokens[there, slot * k_rows : (slot + 1) * k_rows] = normed.astype(BF)
        pick_row = lax.broadcasted_iota(jnp.int32, (n_tp * HEADS, n_tp * width_own), 0)
        pick_col = lax.broadcasted_iota(jnp.int32, (n_tp * HEADS, n_tp * width_own), 1)
        picked = (pick_col // width_own) * HEADS + (
            t * (width_own // HEAD) + (pick_col % width_own) // HEAD
        )
        pick[...] = jnp.where(pick_row == picked, 1.0, 0.0).astype(BF)
        for copy in loads[2:]:
            copy.wait()

        pl.semaphore_wait(barrier, n_tp - 1 + 1)

        def z_items(step):
            return [(m, part) for m in (1, 2, 0) for part in ((1, 0) if step < half else (0,))]

        def z_push(step, m, part):
            ref = others if part else weights
            send(
                w_piece(ref, slot_at(step - 1), m), w_piece(ref, slot_at(step), m),
                z_send.at[step - 1, m, part], z_recv.at[step - 1, m, part], at_sp(onto),
            )

        def z_step(step):
            for m, part in z_items(step):
                piece = w_piece(others if part else weights, slot_at(step), m)
                arrived(piece, z_recv.at[step - 1, m, part])
                if step < half and (m, part) in z_items(step + 1):
                    z_push(step + 1, m, part)
                if part:
                    send(
                        piece, w_piece(weights, slot_at(step), m), d_send.at[step - 1, m],
                        d_recv.at[step - 1, m], at_tp(partner),
                    )

        def z_beside(step):
            for m, part in z_items(step):
                if part:
                    arrived(w_piece(weights, slot_beside(step), m), d_recv.at[step - 1, m])

        def zo_parts(step):
            return (1, 0) if step < half else (0,)

        def zo_push(step, part):
            block = partner if part else t
            send(
                w_out.at[block, slot_at(step - 1)], w_out.at[block, slot_at(step)],
                zo_send.at[step - 1, part], zo_recv.at[step - 1, part], at_sp(onto),
            )

        def zo_step(step):
            if step == 0:
                for part in (1, 0):
                    zo_push(1, part)
                return
            for part in zo_parts(step):
                piece = w_out.at[partner if part else t, slot_at(step)]
                arrived(piece, zo_recv.at[step - 1, part])
                if step < half and part in zo_parts(step + 1):
                    zo_push(step + 1, part)
                send(
                    piece, piece, do_send.at[step - 1, part], do_recv.at[step - 1, part],
                    at_tp(partner),
                )

        def zo_beside(step, part):
            arrived(w_out.at[t if part else partner, slot_beside(step)], do_recv.at[step - 1, part])

        for m, part in z_items(1):
            z_push(1, m, part)

        def tok_piece(block, p):
            return tokens.at[
                pl.ds(pl.multiple_of(block * span + p * piece_rows, piece_rows), piece_rows), :
            ]

        def wo_piece(block, p):
            return w_out.at[block, pl.ds(p * piece_chunks, piece_chunks)]

        class Ring:
            def __init__(self, piece, send_sem, recv_sem, left_first, onward):
                self.piece, self.send_sem, self.recv_sem = piece, send_sem, recv_sem
                self.count = 0
                onward_right, onward_left = onward
                self.onward_right, self.onward_left = onward_right, onward_left
                self.from_left = [(left, p) for p in range(PIECES)] + [
                    (across, p) for p in onward_right
                ]
                self.from_right = [(right, p) for p in left_first] + [
                    (across, p) for p in onward_left
                ]

            def push(self, block, p, where):
                send(
                    self.piece(block, p), self.piece(block, p),
                    self.send_sem.at[self.count], self.recv_sem.at[block, p], at_tp(where),
                )
                self.count += 1

            def take(self, j):
                for number, (block, p) in enumerate((self.from_left[j], self.from_right[j])):
                    arrived(self.piece(block, p), self.recv_sem.at[block, p])
                    if number == 0 and j < PIECES and p in self.onward_right:
                        self.push(block, p, right)
                    if number == 1 and j < PIECES and p in self.onward_left:
                        self.push(block, p, left)
                    self.push(block, p, partner)

            def partners(self, chips):
                for where in chips:
                    block = ((chip + where) % n_chips) * 2 + 1 - core
                    for p in range(PIECES):
                        arrived(self.piece(block, p), self.recv_sem.at[block, p])

        for i in range(1, n_tp):
            send(
                ext_all.at[t], ext_all.at[t], ext_send.at[i], ext_recv.at[t],
                at_tp((t + i) % n_tp),
            )
        tok_ring = Ring(tok_piece, tok_send, tok_recv, (2, 3, 0, 1), ((0, 1), (2, 3)))
        for p, q in zip((0, 1, 2, 3), (2, 3, 0, 1)):
            tok_ring.push(t, p, right)
            tok_ring.push(t, q, left)
        for p in range(PIECES):
            tok_ring.push(t, p, partner)
        wo_ring = Ring(wo_piece, wo_send, wo_recv, (0, 1, 2, 3), ((0, 1), (2, 3)))

        ready = [((p + 1) * piece_chunks) // 2 for p in range(PIECES)]
        pushed = [0, 0]

        def wo_advance(step):
            while pushed[0] < PIECES and ready[pushed[0]] < step:
                while pushed[1] < ready[pushed[0]]:
                    pushed[1] += 1
                    for part in reversed(zo_parts(pushed[1])):
                        zo_beside(pushed[1], part)
                wo_ring.push(t, pushed[0], right)
                wo_ring.push(t, pushed[0], left)
                pushed[0] += 1
            if step <= half:
                zo_step(step)

        reached = [0]

        def wo_go(last):
            while reached[0] <= last:
                wo_advance(reached[0])
                reached[0] += 1

        def project(block, first_slot, last_slot):
            rows = slice(block * 2 * span, (block + 1) * 2 * span)
            part = slice(first_slot * k_rows, last_slot * k_rows)
            early[rows, :] = mm(tokens[rows, part], weights[part, :])

        n_most = n_sp - 3

        wo_go(0)

        row_i = lax.broadcasted_iota(jnp.int32, (2 * BLOCK, 2 * BLOCK), 0)
        col_i = lax.broadcasted_iota(jnp.int32, (2 * BLOCK, 2 * BLOCK), 1)
        causal = jnp.logical_and(row_i >= col_i, row_i // BLOCK == col_i // BLOCK)
        tri = jnp.where(causal, 1.0, 0.0).astype(BF)
        tri3 = jnp.concatenate([tri, tri, tri], axis=1)
        def extra_sums():
            values = ext_all[...].reshape(n_tp * HEADS, span)
            sums = mm(jnp.concatenate(split3(values), axis=1), tri3, NT)
            sums = split3(sums.T)
            for i in range(n_tp):
                chosen = pick[:, i * width_own : (i + 1) * width_own]
                cums[i * span : (i + 1) * span, :] = mm(
                    jnp.concatenate(sums, axis=1), jnp.concatenate([chosen] * 3, axis=0)
                )

        taken = 0
        for step in range(1, half):
            z_step(step)
            wo_go(step)
            while taken < 6 and (taken < step or step == half - 1):
                tok_ring.take(taken)
                taken += 1
        tok_ring.partners((0, 1, n_chips - 1, 2))
        for step in range(1, half - 1):
            z_beside(step)
        for i in range(1, n_tp):
            arrived(ext_all.at[(t + i) % n_tp], ext_recv.at[(t + i) % n_tp])
        extra_sums()
        for block in range(n_chips):
            project(block, 0, n_most)
        z_step(half)
        z_beside(half - 1)
        wo_go(half)
        rest = slice(n_most * k_rows, n_sp * k_rows)
        rows_step = 256
        for r in range(0, rows_all, rows_step):
            rows = slice(r, r + rows_step)
            raw[rows, :] = (early[rows, :] + mm(tokens[rows, rest], weights[rest, :])).astype(BF)

        gaps = gap_in[...].reshape(1, n_tp * width_own)
        gains = hgain_in[...].astype(F32).reshape(1, n_tp * width_own)
        gap, head_gain = gaps[:, :width_own], gains[:, :width_own]
        for i in range(1, n_tp):
            cols = slice(i * width_own, (i + 1) * width_own)
            gap = jnp.where(t == i, gaps[:, cols], gap)
            head_gain = jnp.where(t == i, gains[:, cols], head_gain)
        for i in range(n_tp):
            here = slice(i * span, (i + 1) * span)
            forget = raw[here, width_own : 2 * width_own].astype(F32)
            key = gap / (1.0 + jnp.exp(forget))
            kept = mm(tri3, jnp.concatenate(split3(jnp.log1p(-key)), axis=0))
            cums[here, :] = cums[here, :] + kept
            keys[here, :] = key

        wo_go(half + 1)
        wo_ring.take(0)
        wo_ring.take(1)
        lane = lax.broadcasted_iota(jnp.int32, (HEAD, width_own), 1)
        first = lane < HEAD
        state = jnp.zeros((HEAD, width_own), F32)
        offset = jnp.zeros((1, width_own), F32)
        for b in range(n_blocks):
            here = slice(b * BLOCK, (b + 1) * BLOCK)
            total = cums[(b + 1) * BLOCK - 1 : (b + 1) * BLOCK, :]
            tail = (keys[here, :] * jnp.exp(total - cums[here, :])).astype(BF)
            added = mm(raw[here, 2 * width_own :], tail, TN)
            entering[b] = state.astype(BF)
            offsets[b] = offset
            state = state * jnp.exp(total) + jnp.where(first, added[:HEAD], added[HEAD:])
            offset = offset + total
        log_row = lax.broadcasted_iota(jnp.int32, (LOG_ROWS, width_own), 0)

        def pack(ref, value, logs):
            ref[:HEAD] = value.astype(BF)
            high, middle, low = split3(logs)
            ref[HEAD:] = jnp.where(
                log_row == 0, high.astype(F32),
                jnp.where(log_row == 1, middle.astype(F32),
                          jnp.where(log_row == 2, low.astype(F32), 0.0)),
            ).astype(BF)

        def unpack(ref):
            logs = ref[HEAD:].astype(F32)
            return ref[:HEAD].astype(F32), logs[0:1] + logs[1:2] + logs[2:3]

        pair_copy = pltpu.make_async_remote_copy(
            src_ref=own_state, dst_ref=pair_in, send_sem=pair_send, recv_sem=pair_recv,
            device_id=at_sp((s + 1) % n_sp), device_id_type=MESH,
        )

        def state_copy(j):
            return pltpu.make_async_remote_copy(
                src_ref=pair_state, dst_ref=states.at[s // 2], send_sem=st_send.at[j],
                recv_sem=st_recv.at[s // 2], device_id=at_sp(j), device_id_type=MESH,
            )

        def state_push(k, carry):
            state_copy(n_sp - 1 - k).start()
            return carry

        @pl.when(s % 2 == 0)
        def _():
            pack(own_state, state, offset)
            pair_copy.start()

        @pl.when(s % 2 == 1)
        def _():
            pair_copy.wait_recv()
            value, logs = unpack(pair_in)
            pack(pair_state, value * jnp.exp(offset) + state, logs + offset)
            lax.fori_loop(0, n_sp - 1 - s, state_push, 0)

        wo_ring.take(2)
        lane2 = lax.broadcasted_iota(jnp.int32, (span, width_own), 1)
        first2 = lane2 < HEAD

        def spread_heads(value, mask):
            zero = jnp.zeros_like(value)
            return jnp.concatenate(
                [jnp.where(mask, value, zero), jnp.where(mask, zero, value)], axis=0
            )

        for i in range(n_tp):
            here = slice(i * span, (i + 1) * span)
            query = raw[here, :width_own].astype(F32)
            query = query / (1.0 + jnp.exp(-query))
            cumul = cums[here, :]
            q_decayed = query * jnp.exp(cumul)
            k_decayed = (keys[here, :] * jnp.exp(-cumul)).astype(BF)
            scores = mm(spread_heads(q_decayed, first2).astype(BF), k_decayed, NT)
            scores = jnp.where(jnp.concatenate([causal, causal], axis=0), scores, 0.0)
            within = mm(scores.astype(BF), raw[here, 2 * width_own :])
            within = jnp.where(first2, within[:span], within[span:])
            for j in range(span // BLOCK):
                b = i * (span // BLOCK) + j
                part = slice(j * BLOCK, (j + 1) * BLOCK)
                q_part = q_decayed[part]
                seen = mm(
                    q_part.astype(BF), spread_heads(entering[b].astype(F32), first).astype(BF), NT
                )
                rows = slice(b * BLOCK, (b + 1) * BLOCK)
                local_out[rows, :] = within[part] + seen
                q_glob[rows, :] = (q_part * jnp.exp(offsets[b])).astype(BF)

        wo_ring.take(3)
        wo_ring.take(4)

        pad[...] = jnp.zeros_like(pad)
        pad[:, :HEAD] = init_in[...]
        carried = pad[...].T[:HEAD]

        def advance(j, value):
            arrived(states.at[j], st_recv.at[j])
            added, logs = unpack(states.at[j])
            return value * jnp.exp(logs) + added

        def advance_one(j, value):
            added, logs = unpack(pair_in)
            return value * jnp.exp(logs) + added

        carried = lax.fori_loop(0, s // 2, advance, carried)
        carried = lax.fori_loop(0, s % 2, advance_one, carried)
        prefix[...] = spread_heads(carried, first).astype(BF)

        ones_row = lax.broadcasted_iota(jnp.int32, (width_own, width_own), 0)
        ones_col = lax.broadcasted_iota(jnp.int32, (width_own, width_own), 1)
        same = jnp.where(ones_row // HEAD == ones_col // HEAD, 1.0 / HEAD, 0.0).astype(BF)
        same2 = jnp.concatenate([same, same], axis=0)
        targets = [
            ((chip + where) % n_chips) * 2 + side
            for where in (2, 1, n_chips - 1, 0) for side in (core, 1 - core)
        ]
        targets = targets[:6] + [partner, t]

        def gate(group, first_count):
            for block in group:
                rows = pl.ds(pl.multiple_of(block * span, span), span)
                recurrent = local_out[rows, :] + mm(q_glob[rows, :], prefix[...], NT)
                square = recurrent * recurrent
                high = square.astype(BF)
                low = (square - high.astype(F32)).astype(BF)
                power = mm(jnp.concatenate([high, low], axis=1), same2)
                done = (recurrent * lax.rsqrt(power + EPSILON) * head_gain).astype(BF)
                if block is t:
                    gated_in[:, lanes] = done
                else:
                    gated[rows, :] = done
            for count, block in enumerate(group, first_count):
                if block is t:
                    continue
                rows = pl.ds(pl.multiple_of(block * span, span), span)
                send(
                    gated.at[rows, :], gated_in.at[:, lanes], g_send.at[count],
                    g_recv.at[t], at_tp(block),
                )

        gate(targets[:4], 0)
        part_rows = HEAD // n_tp

        def final_copies(act):
            for h in range(HEADS // n_tp):
                head = t * (HEADS // n_tp) + h
                for i in range(n_tp):
                    copy = pltpu.make_async_remote_copy(
                        src_ref=final_buf.at[pl.ds(h * HEAD + i * part_rows, part_rows), :],
                        dst_ref=final_in, send_sem=f_send.at[h, i], recv_sem=f_recv,
                        device_id={"sp": head, "tp": i}, device_id_type=MESH,
                    )
                    keeps = jnp.logical_and(head == s, t == i)
                    if act == "start":
                        pl.when(jnp.logical_not(keeps))(copy.start)

                        @pl.when(keeps)
                        def _():
                            final_in[...] = final_buf[
                                h * HEAD + i * part_rows : h * HEAD + (i + 1) * part_rows, :
                            ]
                    else:
                        pl.when(jnp.logical_not(keeps))(copy.wait_send)

        if HEADS == n_sp:

            @pl.when(s == n_sp - 1)
            def _():
                last = carried * jnp.exp(offset) + state
                final_buf[...] = jnp.concatenate([last, last], axis=0).T
                final_copies("start")

        gate(targets[4:], 4)
        wo_ring.take(5)
        wo_ring.partners((1, n_chips - 1, 2))
        for step in range(1, half + 1):
            for part in zo_parts(step):
                if step > pushed[1]:
                    zo_beside(step, part)
        for i in range(1, n_tp):
            other = (t + i) % n_tp
            arrived(
                gated_in.at[:, pl.ds(pl.multiple_of(other * width_own, width_own), width_own)],
                g_recv.at[other],
            )

        for pair in range(n_sp // 2):
            right_side = jnp.concatenate(
                [w_out[:, slot].reshape(n_tp * width_own, -1) for slot in (2 * pair, 2 * pair + 1)],
                axis=1,
            )
            product = mm(gated_in[...], right_side).astype(BF)
            cols = product.shape[1] // 2
            for k in range(2):
                source = source_of(2 * pair + k)
                mixed_ref[:, pl.ds(pl.multiple_of(source * cols, cols), cols)] = (
                    product[:, k * cols : (k + 1) * cols]
                )
        if HEADS == n_sp:

            @pl.when(s == n_sp - 1)
            def _():
                final_copies("end")

            keeper = jnp.logical_and(s == n_sp - 1, t == s // (HEADS // n_tp))

            @pl.when(jnp.logical_not(keeper))
            def _():
                arrived(final_in, f_recv)

            for r in range(part_rows):
                final_ref[:, r * HEAD : (r + 1) * HEAD] = final_in[r : r + 1, :HEAD]

        def state_end(k, carry):
            state_copy(n_sp - 1 - k).wait_send()
            return carry

        pl.when(s % 2 == 0)(pair_copy.wait_send)

        @pl.when(s % 2 == 1)
        def _():
            lax.fori_loop(0, n_sp - 1 - s, state_end, 0)

        for copy in sent:
            copy.wait_send()

    return kernel


def solution(mesh):
    n_sp, n_tp = mesh.shape["sp"], mesh.shape["tp"]

    def body(
        tokens, norm_gain, w_query, w_forget, w_input, floor_gap, extra_decay, init_state,
        head_norm_gain, w_output,
    ):
        span, d_model = tokens.shape[1], tokens.shape[2]
        width = w_query.shape[1]
        own = width // n_tp
        rows = n_tp * span
        blocks = rows // BLOCK
        flat = HEADS * HEAD * HEAD // (n_sp * n_tp)
        vmem = pl.BlockSpec(memory_space=pltpu.VMEM)
        hbm = pl.BlockSpec(memory_space=pltpu.HBM)
        half = n_sp // 2
        dma = pltpu.SemaphoreType.DMA
        mixed, final_state = pl.pallas_call(
            make_kernel(n_sp, n_tp, span, own, d_model),
            out_shape=(
                pltpu.VMEM((span, d_model), BF),
                pltpu.VMEM((1, flat), F32),
            ),
            in_specs=[hbm] * 10,
            out_specs=(vmem, vmem),
            scratch_shapes=[
                pltpu.VMEM((span, d_model), BF),
                pltpu.VMEM((d_model,), BF),
                pltpu.VMEM((1, d_model), F32),
                pltpu.VMEM((width,), F32),
                pltpu.VMEM((width,), BF),
                pltpu.VMEM((own, HEAD), F32),
                pltpu.VMEM((rows, d_model), BF),
                pltpu.VMEM((d_model, 3 * own), BF),
                pltpu.VMEM((d_model, 3 * own), BF),
                pltpu.VMEM((n_tp, n_sp, own, d_model // n_sp), BF),
                pltpu.VMEM((n_tp, HEADS, span), F32),
                pltpu.VMEM((span, own), F32),
                pltpu.VMEM((n_tp * HEADS, n_tp * own), BF),
                pltpu.VMEM((rows, 3 * own), F32),
                pltpu.VMEM((rows, 3 * own), BF),
                pltpu.VMEM((rows, own), F32),
                pltpu.VMEM((rows, own), F32),
                pltpu.VMEM((blocks, HEAD, own), BF),
                pltpu.VMEM((blocks, 1, own), F32),
                pltpu.VMEM((rows, own), F32),
                pltpu.VMEM((rows, own), BF),
                pltpu.VMEM((HEAD + LOG_ROWS, own), BF),
                pltpu.VMEM((HEAD + LOG_ROWS, own), BF),
                pltpu.VMEM((HEAD + LOG_ROWS, own), BF),
                pltpu.VMEM((n_sp // 2, HEAD + LOG_ROWS, own), BF),
                pltpu.VMEM((rows, own), BF),
                pltpu.VMEM((span, width), BF),
                pltpu.VMEM((own, 2 * HEAD), F32),
                pltpu.VMEM((HEAD // n_tp, 2 * HEAD), F32),
                pltpu.VMEM((own, own), BF),
                dma((14,)),
                dma((28,)), dma((n_tp, PIECES)), dma((28,)), dma((n_tp, PIECES)),
                dma((half, 3, 2)), dma((half, 3, 2)), dma((half, 2)), dma((half, 2)),
                dma((half, 3)), dma((half, 3)), dma((half, 2)), dma((half, 2)),
                dma((n_tp,)), dma((n_tp,)),
                dma, dma, dma((n_sp,)), dma((n_sp // 2,)),
                dma((n_tp,)), dma((n_tp,)),
                dma((HEADS // n_tp, n_tp)), dma,
            ],
            compiler_params=pltpu.CompilerParams(
                collective_id=0, has_side_effects=True, vmem_limit_bytes=56 * 1024 * 1024
            ),
            name="mixer",
        )(
            tokens.reshape(span, d_model),
            norm_gain,
            w_query, w_forget, w_input,
            floor_gap,
            jnp.swapaxes(extra_decay, 1, 2).reshape(HEADS, span),
            init_state.reshape(HEADS * HEAD, HEAD),
            head_norm_gain,
            w_output,
        )
        return mixed.reshape(1, span, d_model), final_state

    in_specs = (
        P("grp", ("sp", "tp"), None),
        P(),
        P("sp", None),
        P("sp", None),
        P("sp", None),
        P(),
        P("grp", ("sp", "tp"), None),
        P("grp", None, None, None),
        P(),
        P(None, "sp"),
    )
    out_specs = (P("grp", ("sp", "tp"), None), P("grp", ("sp", "tp")))
    return jax.shard_map(body, mesh=mesh, in_specs=in_specs, out_specs=out_specs, check_vma=False)
```
